512 devices in a mesh: rep: 64 (over z, y), fs: 4 (over x), tp: 2 (over core).
Axes of the slice: x: 4, y: 8, z: 8, core: 2. Of those that a mesh axis runs over, the one named last changes fastest.
Arguments:
- inputs: bfloat16 [8192, 2048], P(('rep', 'fs', 'tp')), may hold values from -6 to 6
- cotangent: bfloat16 [8192, 2048], P(('rep', 'fs', 'tp')), may hold values from -24 to 24
- norm_gain: float32 [2048], replicated, may hold values from 0.1 to 1.9
- gate_weight: bfloat16 [2048, 2816], P(None, ('fs', 'tp')), may hold values from -0.125 to 0.125
- up_weight: bfloat16 [2048, 2816], P(None, ('fs', 'tp')), may hold values from -0.125 to 0.125
- down_weight: bfloat16 [2816, 2048], P(('fs', 'tp')), may hold values from -0.109375 to 0.109375
Outputs:
- input_grad: bfloat16 [8192, 2048], P(('rep', 'fs', 'tp'))
- gain_grad: float32 [2048], replicated
- down_grad: float32 [2816, 2048], P(('fs', 'tp'), 'rep')
The draws below stay inside these ranges and needn't reach their ends.
All inputs are finite; a program needn't handle non-finite values.
Results may differ from the reference program's by a relative error of at most 0.0066.
Values may be sent and summed in bfloat16 or wider, within the bound.
No kernel may reach another device: no remote copies, remote signals or barrier semaphores. Data moves between devices by JAX's collectives and lax.ppermute only.
A program may use at most 64 MiB of HBM per device.

```python
import jax
import jax.numpy as jnp
from jax import lax

D = 2048
FF = 2816
TOKENS = 8192


def raised(entries, rng, source, target, shards_of, factor):
    def block_of(axis_at):
        return (jnp.arange(entries.shape[axis_at]) // (entries.shape[axis_at] // shards_of)).reshape((-1,) + (1,) * (entries.ndim - 1 - axis_at))

    near = jax.random.permutation(rng, shards_of)[block_of(target)]
    second = (block_of(target) + shards_of // 2) % shards_of
    return jnp.where((block_of(source) == near) | (block_of(source) == second), factor * entries, entries)


def shard_levels(rng, extent, cuts, smallest, top_value):
    loudness = 1.0
    for axis_at, shards_of in cuts:
        steps = jax.random.uniform(jax.random.fold_in(jax.random.fold_in(rng, 6), axis_at), (shards_of,), jnp.float32, smallest / len(cuts), top_value / len(cuts))
        loudness = loudness * jnp.repeat(jnp.exp(steps), extent[axis_at] // shards_of).reshape((-1,) + (1,) * (len(extent) - 1 - axis_at))
    return loudness


def centred(own_key, extent, deviation, limit, shards=(), kind=jnp.bfloat16):
    values = deviation * jax.random.normal(own_key, extent, jnp.float32)
    if shards:
        values = values * shard_levels(own_key, extent, shards, -0.22, 0.18)
    return jnp.clip(values, -limit, limit).astype(kind)


def heavy_noise(stream_key, shape, scale, reach, pieces, heavy, kind=jnp.bfloat16):
    entries = scale * jax.random.normal(stream_key, shape, jnp.float32)
    if pieces:
        entries = entries * shard_levels(stream_key, shape, pieces, -0.22, 0.18)
    return jnp.clip(raised(entries, jax.random.fold_in(stream_key, 3), *heavy), -reach, reach).astype(kind)


def setup_inputs(seed: int = 0) -> dict:
    streams_of = jax.random.split(jax.random.key(seed), 7)
    return {
        "inputs": centred(streams_of[0], (TOKENS, D), 1.0, 6.0, ((0, 512),)),
        "cotangent": heavy_noise(streams_of[1], (TOKENS, D), 1.0, 24.0, ((0, 512),), (0, 1, 512, 6.0)),
        "norm_gain": jnp.clip(1.0 + 0.18 * jax.random.normal(streams_of[2], (D,), jnp.float32), 0.1, 1.9),
        "gate_weight": centred(streams_of[3], (D, FF), D ** -0.5, 0.125, ((1, 8),)),
        "up_weight": centred(streams_of[4], (D, FF), D ** -0.5, 0.125, ((1, 8),)),
        "down_weight": centred(streams_of[5], (FF, D), FF ** -0.5, 0.109375, ((0, 8),)),
    }


EPS = 1e-06

def reference(inputs, cotangent, norm_gain, gate_weight, up_weight, down_weight):
    xf = inputs.astype(jnp.float32)
    inv = lax.rsqrt(lax.optimization_barrier(jnp.mean(xf * xf, axis=-1, keepdims=True)) + EPS)
    normed = xf * inv
    hidden_in = (normed * norm_gain).astype(jnp.bfloat16)
    gate = jnp.dot(hidden_in, gate_weight, preferred_element_type=jnp.float32)
    up = jnp.dot(hidden_in, up_weight, preferred_element_type=jnp.float32)
    sig = jax.nn.sigmoid(gate)
    act = gate * sig
    hidden = (act * up).astype(jnp.bfloat16)
    d_hidden = 0.5 * jnp.dot(cotangent, down_weight.T, preferred_element_type=jnp.float32)
    d_gate = (d_hidden * up * sig * (1.0 + gate * (1.0 - sig))).astype(jnp.bfloat16)
    d_up = (d_hidden * act).astype(jnp.bfloat16)
    down_grad = 0.5 * jnp.dot(hidden.T, cotangent, preferred_element_type=jnp.float32)
    d_in = jnp.dot(d_gate, gate_weight.T, preferred_element_type=jnp.float32) + jnp.dot(d_up, up_weight.T, preferred_element_type=jnp.float32)
    gain_grad = lax.optimization_barrier(jnp.sum(d_in * normed, axis=0))
    scaled = d_in * norm_gain
    input_grad = (inv * (scaled - normed * lax.optimization_barrier(jnp.mean(scaled * normed, axis=-1, keepdims=True)))).astype(jnp.bfloat16)
    return (input_grad, gain_grad, down_grad)
```

```python
import jax
import jax.numpy as jnp
import numpy as np
from jax import lax
from jax.experimental import pallas as pl
from jax.experimental.pallas import tpu as pltpu
from jax.sharding import PartitionSpec as P

EPS = 1e-06
SIDE = 8
HALF = SIDE // 2
EVERY = ("rep", "fs", "tp")
OWN = ("fs", "tp")


def place(label, high):
    return 2 * high + (label ^ (high // 2))


QUADS = [
    [place(a, zh) * SIDE + place(b, yh) for a in range(2) for b in range(2)]
    for zh in range(HALF)
    for yh in range(HALF)
]
FAR = [
    [place(a, zh) * SIDE + place(b, yh) for zh in range(HALF) for yh in range(HALF)]
    for a in range(2)
    for b in range(2)
]


def one_row_of_quads():
    order = np.concatenate(
        [
            np.arange(32) + 32 * place(b, yh)
            for b in range(2)
            for yh in range(HALF)
        ]
    )
    return np.eye(256, dtype=np.float32)[:, order]


def nt(left, right):
    return lax.dot_general(
        left, right, (((1,), (1,)), ((), ())), preferred_element_type=jnp.float32
    )


def tn(left, right):
    return lax.dot_general(
        left, right, (((0,), (0,)), ((), ())), preferred_element_type=jnp.float32
    )


def nn(left, right):
    return jnp.dot(left, right, preferred_element_type=jnp.float32)


def local_kernel(near, far, gain, pick, gate_w, up_w, down_w, sent, keep, give, gain_sum):
    xf = jnp.concatenate((near[:, :2048], far[:, :2048]), axis=0).astype(jnp.float32)
    dy = jnp.concatenate((near[:, 2048:], far[:, 2048:]), axis=0)
    inv = lax.rsqrt(jnp.mean(xf * xf, axis=-1, keepdims=True) + EPS)
    normed = xf * inv
    hidden_in = (normed * gain[...]).astype(jnp.bfloat16)
    gate = nt(hidden_in, gate_w[...])
    up = nt(hidden_in, up_w[...])
    sig = 1.0 / (1.0 + jnp.exp(-gate))
    act = gate * sig
    hidden = (act * up).astype(jnp.bfloat16)
    d_hidden = 0.5 * nt(dy, down_w[...])
    d_gate = (d_hidden * up * sig * (1.0 + gate * (1.0 - sig))).astype(jnp.bfloat16)
    d_up = (d_hidden * act).astype(jnp.bfloat16)
    part = nn(d_gate, gate_w[...]) + nn(d_up, up_w[...])
    keep[...] = part[:64]
    give[...] = part[64:].astype(jnp.bfloat16)
    total = jnp.sum(part * normed, axis=0, keepdims=True)
    for k in range(8):
        gain_sum[k : k + 1, :] = total[:, 256 * k : 256 * k + 256]
    for z in range(SIDE):
        zh = z // 2
        a = (z % 2) ^ (zh // 2)
        turned = nn(dy[:, 256 * z : 256 * z + 256], pick[...]).astype(jnp.bfloat16)
        for b in range(2):
            sent[2 * a + b, :128, 128 * zh : 128 * zh + 128] = turned[:, 128 * b : 128 * b + 128]
    for p in range(4):
        sent[p, :128, 512:864] = hidden
        sent[p, :128, 864:] = jnp.zeros((128, 32), jnp.bfloat16)
        sent[p, 128:, :] = jnp.zeros((16, 896), jnp.bfloat16)


def reduce_kernel(got, blocks):
    part = tn(got[0, :128, :512], got[0, :128, 512:])
    for p in range(1, 4):
        part = part + tn(got[p, :128, :512], got[p, :128, 512:])
    part = part.astype(jnp.bfloat16)
    total = jnp.zeros((16, 256), jnp.float32)
    for p in range(4):
        total = total + got[p, 128:, :256].astype(jnp.float32)
    total = total.astype(jnp.bfloat16)
    for k in range(16):
        blocks[k, :32, :] = part[32 * k : 32 * k + 32, :]
        blocks[k, 32:, :256] = total
        blocks[k, 32:, 256:] = jnp.zeros((16, 128), jnp.bfloat16)


def last_kernel(got, down, gain):
    total = got[0].astype(jnp.float32)
    for k in range(1, 16):
        total = total + got[k].astype(jnp.float32)
    down[...] = 0.5 * total[:32, :352]
    for k in range(8):
        gain[:, 256 * k : 256 * k + 256] = total[32 + k : 33 + k, :256]


def call(body, shapes, *args, flops=1000000):
    whole = pl.BlockSpec(memory_space=pltpu.VMEM)
    out = [jax.ShapeDtypeStruct(s, t) for s, t in shapes]
    return pl.pallas_call(
        body,
        out_shape=out,
        in_specs=[whole] * len(args),
        out_specs=[whole] * len(out),
        cost_estimate=pl.CostEstimate(flops=flops, bytes_accessed=4000000, transcendentals=0),
    )(*args)


def to_all(array, axis):
    count = lax.axis_size(axis)
    return lax.all_to_all(
        jnp.broadcast_to(array[None], (count, *array.shape)), axis, 0, 0, tiled=True
    )


def partner(array, axis, bit):
    count = lax.axis_size(axis)
    return lax.ppermute(array, axis, [(i, i ^ bit) for i in range(count)])


def per_device(inputs, cotangent, norm_gain, gate_weight, up_weight, down_weight):
    near = to_all(jnp.concatenate((inputs, cotangent), axis=1), "fs").reshape(64, 4096)
    other = partner(near, "tp", 1)
    pick = jnp.asarray(one_row_of_quads(), jnp.bfloat16)
    sent, keep, give, part_gain = call(
        local_kernel,
        [
            ((4, 144, 896), jnp.bfloat16),
            ((64, 2048), jnp.float32),
            ((64, 2048), jnp.bfloat16),
            ((8, 256), jnp.float32),
        ],
        near,
        other,
        norm_gain.reshape(1, 2048),
        pick,
        gate_weight.T,
        up_weight.T,
        down_weight,
        flops=1000000000,
    )

    group_gain = jnp.sum(to_all(part_gain, OWN).reshape(8, 8, 256), axis=0)
    rows = jnp.broadcast_to(group_gain.astype(jnp.bfloat16)[None], (4, 8, 256))
    sent = lax.dynamic_update_slice(sent, rows, (0, 128, 0))
    got = lax.all_to_all(sent, "rep", 0, 0, tiled=True, axis_index_groups=QUADS)
    (blocks,) = call(reduce_kernel, [((16, 48, 384), jnp.bfloat16)], got)
    got = lax.all_to_all(blocks, "rep", 0, 0, tiled=True, axis_index_groups=FAR)
    down, gain = call(last_kernel, [((32, 352), jnp.float32), ((1, 2048), jnp.float32)], got)
    down_grad = down.T
    gain_grad = gain.reshape(2048)

    chip_in = keep + partner(give, "tp", 1).astype(jnp.float32)
    me = lax.axis_index("fs")
    odd = lax.rem(me, 2)
    pairs = chip_in.reshape(2, 2, 16, 2048)
    mine = lax.dynamic_index_in_dim(pairs, odd, 1, keepdims=False)
    give = lax.dynamic_index_in_dim(pairs, 1 - odd, 1, keepdims=False)
    mine = mine + partner(give.astype(jnp.bfloat16), "fs", 1).astype(jnp.float32)
    high = me // 2
    give = lax.dynamic_index_in_dim(mine, 1 - high, 0, keepdims=False)
    mine = lax.dynamic_index_in_dim(mine, high, 0, keepdims=False)
    d_in = mine + partner(give.astype(jnp.bfloat16), "fs", 2).astype(jnp.float32)

    own_xf = inputs.astype(jnp.float32)
    own_inv = lax.rsqrt(jnp.mean(own_xf * own_xf, axis=-1, keepdims=True) + EPS)
    own_normed = own_xf * own_inv
    scaled = d_in * norm_gain
    input_grad = (
        own_inv * (scaled - own_normed * jnp.mean(scaled * own_normed, axis=-1, keepdims=True))
    ).astype(jnp.bfloat16)
    return (input_grad, gain_grad, down_grad)


def solution(mesh):
    placed = (
        P(EVERY, None),
        P(EVERY, None),
        P(),
        P(None, OWN),
        P(None, OWN),
        P(OWN, None),
    )
    return jax.shard_map(
        per_device,
        mesh=mesh,
        in_specs=placed,
        out_specs=(P(EVERY, None), P(), P(OWN, "rep")),
        check_vma=False,
    )
```

```python
import jax
import jax.numpy as jnp
import numpy as np
from jax import lax
from jax.experimental import pallas as pl
from jax.experimental.pallas import tpu as pltpu
from jax.sharding import PartitionSpec as P


EPS = 1e-06
SIDE = 8
HALF = SIDE // 2
EVERY = ("rep", "fs", "tp")
OWN = ("fs", "tp")


def place(label, high):
    return 2 * high + (label ^ (high // 2))


QUADS = [
    [place(a, zh) * SIDE + place(b, yh) for a in range(2) for b in range(2)]
    for zh in range(HALF)
    for yh in range(HALF)
]
QUAD_DEVICES = [[8 * r + k for r in quad for k in range(8)] for quad in QUADS]
FAR = [
    [place(a, zh) * SIDE + place(b, yh) for zh in range(HALF) for yh in range(HALF)]
    for a in range(2)
    for b in range(2)
]


def one_row_of_quads():
    order = np.concatenate(
        [
            np.arange(32) + 32 * place(b, yh)
            for b in range(2)
            for yh in range(HALF)
        ]
    )
    return np.eye(256, dtype=np.float32)[:, order]


def nt(left, right):
    return lax.dot_general(
        left, right, (((1,), (1,)), ((), ())), preferred_element_type=jnp.float32
    )


def tn(left, right):
    return lax.dot_general(
        left, right, (((0,), (0,)), ((), ())), preferred_element_type=jnp.float32
    )


def nn(left, right):
    return jnp.dot(left, right, preferred_element_type=jnp.float32)


def my_label():
    me = lax.axis_index("rep")
    z, y = me // SIDE, lax.rem(me, SIDE)
    a = lax.rem(z, 2) ^ (z // HALF)
    b = lax.rem(y, 2) ^ (y // HALF)
    return 2 * a + b


def local_kernel(
    near, far, gain, pick, gate_hbm, up_hbm, down_hbm, own, sent_y, sent_z, sent_zy, keep, give,
    gain_sum, turned, gate_w, up_w, down_w, sems,
):
    loads = [
        pltpu.make_async_copy(source, target, sems.at[k])
        for k, (source, target) in enumerate(
            ((gate_hbm, gate_w), (up_hbm, up_w), (down_hbm, down_w))
        )
    ]
    for load in loads:
        load.start()
    xf = jnp.concatenate((near[:, :2048], far[:, :2048]), axis=0).astype(jnp.float32)
    dy = jnp.concatenate((near[:, 2048:], far[:, 2048:]), axis=0)
    inv = lax.rsqrt(jnp.mean(xf * xf, axis=-1, keepdims=True) + EPS)
    normed = xf * inv
    hidden_in = (normed * gain[...]).astype(jnp.bfloat16)
    for z in range(SIDE):
        zh = z // 2
        a = (z % 2) ^ (zh // 2)
        block = nn(dy[:, 256 * z : 256 * z + 256], pick[...]).astype(jnp.bfloat16)
        for b in range(2):
            turned[2 * a + b, :, 128 * zh : 128 * zh + 128] = block[:, 128 * b : 128 * b + 128]
    loads[0].wait()
    gate = nt(hidden_in, gate_w[...])
    loads[1].wait()
    up = nt(hidden_in, up_w[...])
    sig = 1.0 / (1.0 + jnp.exp(-gate))
    act = gate * sig
    hidden = (act * up).astype(jnp.bfloat16)
    loads[2].wait()
    d_hidden = 0.5 * nt(dy, down_w[...])
    d_gate = (d_hidden * up * sig * (1.0 + gate * (1.0 - sig))).astype(jnp.bfloat16)
    d_up = (d_hidden * act).astype(jnp.bfloat16)
    part = nn(d_gate, gate_w[...]) + nn(d_up, up_w[...])
    keep[...] = part[:64]
    give[...] = part[64:].astype(jnp.bfloat16)
    total = jnp.sum(part * normed, axis=0, keepdims=True)
    rows = jnp.concatenate([total[:, 256 * k : 256 * k + 256] for k in range(8)], axis=0)
    for k in range(32):
        gain_sum[k] = rows.astype(jnp.bfloat16)
    mine = my_label()
    for k, out in enumerate((own, sent_y, sent_z, sent_zy)):
        out[:, :512] = turned[mine ^ k]
        out[:, 512:864] = hidden
        out[:, 864:] = jnp.zeros((128, 32), jnp.bfloat16)


def reduce_kernel(own, got_y, got_z, got_zy, gains, blocks):
    part = tn(own[:, :512], own[:, 512:])
    for got in (got_y, got_z, got_zy):
        part = part + tn(got[:, :512], got[:, 512:])
    total = jnp.sum(gains[...].astype(jnp.float32), axis=0).astype(jnp.bfloat16)
    for k in range(16):
        mine = part[32 * k : 32 * k + 32]
        one, two, three, four = (mine[8 * j : 8 * j + 8, 256:352] for j in range(4))
        rest = jnp.concatenate(
            (
                jnp.concatenate((one, two[:, :32]), axis=1),
                jnp.concatenate((two[:, 32:], three[:, :64]), axis=1),
                jnp.concatenate((three[:, 64:], four), axis=1),
            ),
            axis=0,
        )
        blocks[k, :32] = mine[:, :128].astype(jnp.bfloat16)
        blocks[k, 32:64] = mine[:, 128:256].astype(jnp.bfloat16)
        blocks[k, 64:88] = rest.astype(jnp.bfloat16)
        blocks[k, 88:96] = total[:, :128]
        blocks[k, 96:] = total[:, 128:]


def last_kernel(got, down, gain):
    total = got[0].astype(jnp.float32)
    for k in range(1, 16):
        total = total + got[k].astype(jnp.float32)
    one, two, three = (total[64 + 8 * j : 72 + 8 * j] for j in range(3))
    down[:, :128] = 0.5 * total[:32]
    down[:, 128:256] = 0.5 * total[32:64]
    down[:8, 256:] = 0.5 * one[:, :96]
    down[8:16, 256:] = 0.5 * jnp.concatenate((one[:, 96:], two[:, :64]), axis=1)
    down[16:24, 256:] = 0.5 * jnp.concatenate((two[:, 64:], three[:, :32]), axis=1)
    down[24:, 256:] = 0.5 * three[:, 32:]
    for k in range(8):
        for half in range(2):
            at = 256 * k + 128 * half
            gain[:, at : at + 128] = total[88 + 8 * half + k : 89 + 8 * half + k]


def call(body, shapes, *args, scratch=(), flops=1000000, vmem=16, left=0):
    whole = pl.BlockSpec(memory_space=pltpu.VMEM)
    far = pl.BlockSpec(memory_space=pltpu.HBM)
    out = [jax.ShapeDtypeStruct(s, t) for s, t in shapes]
    return pl.pallas_call(
        body,
        out_shape=out,
        in_specs=[whole] * (len(args) - left) + [far] * left,
        out_specs=[whole] * len(out),
        scratch_shapes=scratch,
        cost_estimate=pl.CostEstimate(flops=flops, bytes_accessed=4000000, transcendentals=0),
        compiler_params=pltpu.CompilerParams(vmem_limit_bytes=vmem * 2**20),
    )(*args)


def to_all(array, axis):
    count = lax.axis_size(axis)
    return lax.all_to_all(
        jnp.broadcast_to(array[None], (count, *array.shape)), axis, 0, 0, tiled=True
    )


def partner(array, axis, bit):
    count = lax.axis_size(axis)
    return lax.ppermute(array, axis, [(i, i ^ bit) for i in range(count)])


def per_device(inputs, cotangent, norm_gain, gate_weight, up_weight, down_weight):
    near = to_all(jnp.concatenate((inputs, cotangent), axis=1), "fs").reshape(64, 4096)
    other = partner(near, "tp", 1)
    pick = jnp.asarray(one_row_of_quads(), jnp.bfloat16)
    block = ((128, 896), jnp.bfloat16)
    own, sent_y, sent_z, sent_zy, keep, give, part_gain = call(
        local_kernel,
        [
            block,
            block,
            block,
            block,
            ((64, 2048), jnp.float32),
            ((64, 2048), jnp.bfloat16),
            ((32, 8, 256), jnp.bfloat16),
        ],
        near,
        other,
        norm_gain.reshape(1, 2048),
        pick,
        *(
            pltpu.with_memory_space_constraint(w, pltpu.HBM)
            for w in (gate_weight.T, up_weight.T, down_weight)
        ),
        scratch=[
            pltpu.VMEM((4, 128, 512), jnp.bfloat16),
            pltpu.VMEM((352, 2048), jnp.bfloat16),
            pltpu.VMEM((352, 2048), jnp.bfloat16),
            pltpu.VMEM((352, 2048), jnp.bfloat16),
            pltpu.SemaphoreType.DMA((3,)),
        ],
        flops=1000000000,
        vmem=32,
        left=3,
    )

    gains = lax.all_to_all(
        part_gain, EVERY, 0, 0, tiled=True, axis_index_groups=QUAD_DEVICES
    )
    got_zy = partner(sent_zy, "rep", SIDE + 1)
    got_z = partner(sent_z, "rep", SIDE)
    got_y = partner(sent_y, "rep", 1)
    (blocks,) = call(
        reduce_kernel,
        [((16, 104, 128), jnp.bfloat16)],
        own,
        got_y,
        got_z,
        got_zy,
        gains,
    )
    got = lax.all_to_all(blocks, "rep", 0, 0, tiled=True, axis_index_groups=FAR)
    down, gain = call(last_kernel, [((32, 352), jnp.float32), ((1, 2048), jnp.float32)], got)
    down_grad = down.T
    gain_grad = gain.reshape(2048)

    got = partner(give, "tp", 1)
    chip_in = keep + got.astype(jnp.float32)
    me = lax.axis_index("fs")
    odd = lax.rem(me, 2)
    pairs = chip_in.reshape(2, 2, 16, 2048)
    mine = lax.dynamic_index_in_dim(pairs, odd, 1, keepdims=False)
    give = lax.dynamic_index_in_dim(pairs, 1 - odd, 1, keepdims=False)
    got = partner(give.astype(jnp.bfloat16), "fs", 1)
    mine = mine + got.astype(jnp.float32)
    high = me // 2
    give = lax.dynamic_index_in_dim(mine, 1 - high, 0, keepdims=False)
    mine = lax.dynamic_index_in_dim(mine, high, 0, keepdims=False)
    got = partner(give.astype(jnp.bfloat16), "fs", 2)
    d_in = mine + got.astype(jnp.float32)

    own_xf = inputs.astype(jnp.float32)
    own_inv = lax.rsqrt(jnp.mean(own_xf * own_xf, axis=-1, keepdims=True) + EPS)
    own_normed = own_xf * own_inv
    scaled = d_in * norm_gain
    input_grad = (
        own_inv * (scaled - own_normed * jnp.mean(scaled * own_normed, axis=-1, keepdims=True))
    ).astype(jnp.bfloat16)
    return (input_grad, gain_grad, down_grad)


def solution(mesh):
    placed = (
        P(EVERY, None),
        P(EVERY, None),
        P(),
        P(None, OWN),
        P(None, OWN),
        P(OWN, None),
    )

    return jax.shard_map(
        per_device,
        mesh=mesh,
        in_specs=placed,
        out_specs=(P(EVERY, None), P(), P(OWN, "rep")),
        check_vma=False,
    )
```

```python
import jax
import jax.numpy as jnp
import numpy as np
from jax import lax
from jax.experimental import pallas as pl
from jax.experimental.pallas import tpu as pltpu
from jax.sharding import PartitionSpec as P


EPS = 1e-06
SIDE = 8
HALF = SIDE // 2
EVERY = ("rep", "fs", "tp")
OWN = ("fs", "tp")


def place(label, high):
    return 2 * high + (label ^ (high // 2))


QUADS = [
    [place(a, zh) * SIDE + place(b, yh) for a in range(2) for b in range(2)]
    for zh in range(HALF)
    for yh in range(HALF)
]
QUAD_DEVICES = [[8 * r + k for r in quad for k in range(8)] for quad in QUADS]
FAR = [
    [place(a, zh) * SIDE + place(b, yh) for zh in range(HALF) for yh in range(HALF)]
    for a in range(2)
    for b in range(2)
]


def one_row_of_quads():
    order = np.concatenate(
        [
            np.arange(32) + 32 * place(b, yh)
            for b in range(2)
            for yh in range(HALF)
        ]
    )
    return np.eye(256, dtype=np.float32)[:, order]


def nt(left, right):
    return lax.dot_general(
        left, right, (((1,), (1,)), ((), ())), preferred_element_type=jnp.float32
    )


def tn(left, right):
    return lax.dot_general(
        left, right, (((0,), (0,)), ((), ())), preferred_element_type=jnp.float32
    )


def nn(left, right):
    return jnp.dot(left, right, preferred_element_type=jnp.float32)


def my_label():
    me = lax.axis_index("rep")
    z, y = me // SIDE, lax.rem(me, SIDE)
    a = lax.rem(z, 2) ^ (z // HALF)
    b = lax.rem(y, 2) ^ (y // HALF)
    return 2 * a + b


def local_kernel(
    near, far, gain, pick, gate_w, up_hbm, down_hbm, own, sent_y, sent_z, sent_zy, keep, give,
    gain_sum, turned, up_w, down_w, gain_rows, sems,
):
    loads = [
        pltpu.make_async_copy(source, target, sems.at[k])
        for k, (source, target) in enumerate(((up_hbm, up_w), (down_hbm, down_w)))
    ]
    mine = my_label()

    once = jnp.minimum(mine, 0) + 1

    @pl.loop(0, once)
    def _(_):
        for load in loads:
            load.start()

    xf = jnp.concatenate((near[:, :2048], far[:, :2048]), axis=0).astype(jnp.float32)
    dy = jnp.concatenate((near[:, 2048:], far[:, 2048:]), axis=0)
    inv = lax.rsqrt(jnp.mean(xf * xf, axis=-1, keepdims=True) + EPS)
    normed = xf * inv
    hidden_in = (normed * gain[...]).astype(jnp.bfloat16)
    for z in range(SIDE):
        zh = z // 2
        a = (z % 2) ^ (zh // 2)
        block = nn(dy[:, 256 * z : 256 * z + 256], pick[...]).astype(jnp.bfloat16)
        for b in range(2):
            turned[2 * a + b, :, 128 * zh : 128 * zh + 128] = block[:, 128 * b : 128 * b + 128]
    gate = nt(hidden_in, gate_w[...])
    loads[0].wait()
    up = nt(hidden_in, up_w[...])
    sig = 1.0 / (1.0 + jnp.exp(-gate))
    act = gate * sig
    hidden = (act * up).astype(jnp.bfloat16)
    loads[1].wait()
    d_hidden = 0.5 * nt(dy, down_w[...])
    d_gate = (d_hidden * up * sig * (1.0 + gate * (1.0 - sig))).astype(jnp.bfloat16)
    d_up = (d_hidden * act).astype(jnp.bfloat16)
    part = nn(d_gate, gate_w[...]) + nn(d_up, up_w[...])
    keep[...] = part[:64]
    give[...] = part[64:].astype(jnp.bfloat16)
    total = jnp.sum(part * normed, axis=0, keepdims=True)
    rows = jnp.concatenate([total[:, 256 * k : 256 * k + 256] for k in range(8)], axis=0)
    for k in range(32):
        gain_rows[k] = rows.astype(jnp.bfloat16)
    store = pltpu.make_async_copy(gain_rows, gain_sum, sems.at[2])

    @pl.loop(0, once)
    def _(_):
        store.start()

    for k, out in enumerate((own, sent_y, sent_z, sent_zy)):
        out[:, :512] = turned[mine ^ k]
        out[:, 512:864] = hidden
        out[:, 864:] = jnp.zeros((128, 32), jnp.bfloat16)
    store.wait()


def reduce_kernel(own, got_y, got_z, got_zy, gains, blocks):
    part = tn(own[:, :512], own[:, 512:])
    for got in (got_y, got_z, got_zy):
        part = part + tn(got[:, :512], got[:, 512:])
    total = jnp.sum(gains[...].astype(jnp.float32), axis=0).astype(jnp.bfloat16)
    for k in range(16):
        mine = part[32 * k : 32 * k + 32]
        one, two, three, four = (mine[8 * j : 8 * j + 8, 256:352] for j in range(4))
        rest = jnp.concatenate(
            (
                jnp.concatenate((one, two[:, :32]), axis=1),
                jnp.concatenate((two[:, 32:], three[:, :64]), axis=1),
                jnp.concatenate((three[:, 64:], four), axis=1),
            ),
            axis=0,
        )
        blocks[k, :32] = mine[:, :128].astype(jnp.bfloat16)
        blocks[k, 32:64] = mine[:, 128:256].astype(jnp.bfloat16)
        blocks[k, 64:88] = rest.astype(jnp.bfloat16)
        blocks[k, 88:96] = total[:, :128]
        blocks[k, 96:] = total[:, 128:]


def last_kernel(got, down, gain):
    total = got[0].astype(jnp.float32)
    for k in range(1, 16):
        total = total + got[k].astype(jnp.float32)
    one, two, three = (total[64 + 8 * j : 72 + 8 * j] for j in range(3))
    down[:, :128] = 0.5 * total[:32]
    down[:, 128:256] = 0.5 * total[32:64]
    down[:8, 256:] = 0.5 * one[:, :96]
    down[8:16, 256:] = 0.5 * jnp.concatenate((one[:, 96:], two[:, :64]), axis=1)
    down[16:24, 256:] = 0.5 * jnp.concatenate((two[:, 64:], three[:, :32]), axis=1)
    down[24:, 256:] = 0.5 * three[:, 32:]
    for k in range(8):
        for half in range(2):
            at = 256 * k + 128 * half
            gain[:, at : at + 128] = total[88 + 8 * half + k : 89 + 8 * half + k]


def split_kernel(keep, got, mine, to_one, to_two, to_three):
    me = lax.axis_index("fs")
    for k, out in enumerate((mine, to_one, to_two, to_three)):
        rows = pl.ds(pl.multiple_of(16 * (me ^ k), 16), 16)
        out[...] = (keep[rows, :] + got[rows, :].astype(jnp.float32)).astype(out.dtype)


def input_kernel(mine, from_one, from_two, from_three, inputs, gain, out):
    d_in = mine[...]
    for got in (from_one, from_two, from_three):
        d_in = d_in + got[...].astype(jnp.float32)
    xf = inputs[...].astype(jnp.float32)
    inv = lax.rsqrt(jnp.mean(xf * xf, axis=-1, keepdims=True) + EPS)
    normed = xf * inv
    scaled = d_in * gain[...]
    mean = jnp.mean(scaled * normed, axis=-1, keepdims=True)
    out[...] = (inv * (scaled - normed * mean)).astype(out.dtype)


def call(body, shapes, *args, scratch=(), flops=1000000, vmem=16, left=0, last=0):
    whole = pl.BlockSpec(memory_space=pltpu.VMEM)
    far = pl.BlockSpec(memory_space=pltpu.HBM)
    out = [jax.ShapeDtypeStruct(s, t) for s, t in shapes]
    return pl.pallas_call(
        body,
        out_shape=out,
        in_specs=[whole] * (len(args) - left) + [far] * left,
        out_specs=[whole] * (len(out) - last) + [far] * last,
        scratch_shapes=scratch,
        cost_estimate=pl.CostEstimate(flops=flops, bytes_accessed=4000000, transcendentals=0),
        compiler_params=pltpu.CompilerParams(vmem_limit_bytes=vmem * 2**20),
    )(*args)


def to_all(array, axis):
    count = lax.axis_size(axis)
    return lax.all_to_all(
        jnp.broadcast_to(array[None], (count, *array.shape)), axis, 0, 0, tiled=True
    )


def partner(array, axis, bit):
    count = lax.axis_size(axis)
    return lax.ppermute(array, axis, [(i, i ^ bit) for i in range(count)])


def per_device(inputs, cotangent, norm_gain, gate_weight, up_weight, down_weight):
    near = to_all(jnp.concatenate((inputs, cotangent), axis=1), "fs").reshape(64, 4096)
    other = partner(near, "tp", 1)
    pick = jnp.asarray(one_row_of_quads(), jnp.bfloat16)
    block = ((128, 896), jnp.bfloat16)
    own, sent_y, sent_z, sent_zy, keep, give, part_gain = call(
        local_kernel,
        [
            block,
            block,
            block,
            block,
            ((64, 2048), jnp.float32),
            ((64, 2048), jnp.bfloat16),
            ((32, 8, 256), jnp.bfloat16),
        ],
        near,
        other,
        norm_gain.reshape(1, 2048),
        pick,
        gate_weight.T,
        pltpu.with_memory_space_constraint(up_weight.T, pltpu.HBM),
        pltpu.with_memory_space_constraint(down_weight, pltpu.HBM),
        scratch=[
            pltpu.VMEM((4, 128, 512), jnp.bfloat16),
            pltpu.VMEM((352, 2048), jnp.bfloat16),
            pltpu.VMEM((352, 2048), jnp.bfloat16),
            pltpu.VMEM((32, 8, 256), jnp.bfloat16),
            pltpu.SemaphoreType.DMA((3,)),
        ],
        flops=1000000000,
        vmem=32,
        left=2,
        last=1,
    )

    gains = lax.all_to_all(
        part_gain, EVERY, 0, 0, tiled=True, axis_index_groups=QUAD_DEVICES
    )
    got_zy = partner(sent_zy, "rep", SIDE + 1)
    got_z = partner(sent_z, "rep", SIDE)
    got_y = partner(sent_y, "rep", 1)
    (blocks,) = call(
        reduce_kernel,
        [((16, 104, 128), jnp.bfloat16)],
        own,
        got_y,
        got_z,
        got_zy,
        gains,
    )
    got = lax.all_to_all(blocks, "rep", 0, 0, tiled=True, axis_index_groups=FAR)
    down, gain = call(last_kernel, [((32, 352), jnp.float32), ((1, 2048), jnp.float32)], got)
    down_grad = down.T
    gain_grad = gain.reshape(2048)

    got = partner(give, "tp", 1)
    tokens = ((16, 2048), jnp.bfloat16)
    mine, *sends = call(
        split_kernel, [((16, 2048), jnp.float32), tokens, tokens, tokens], keep, got
    )
    gots = []
    for k in range(3):
        gots.append(partner(sends[k], "fs", k + 1))
    (input_grad,) = call(
        input_kernel, [tokens], mine, *gots, inputs, norm_gain.reshape(1, 2048)
    )
    return (input_grad, gain_grad, down_grad)


def solution(mesh):
    placed = (
        P(EVERY, None),
        P(EVERY, None),
        P(),
        P(None, OWN),
        P(None, OWN),
        P(OWN, None),
    )

    return jax.shard_map(
        per_device,
        mesh=mesh,
        in_specs=placed,
        out_specs=(P(EVERY, None), P(), P(OWN, "rep")),
        check_vma=False,
    )
```

```python
import jax
import jax.numpy as jnp
import numpy as np
from jax import lax
from jax.experimental import pallas as pl
from jax.experimental.pallas import tpu as pltpu
from jax.sharding import PartitionSpec as P


EPS = 1e-06
SIDE = 8
HALF = SIDE // 2
FIRST_CHIP = 3
EVERY = ("rep", "fs", "tp")
OWN = ("fs", "tp")


def place(label, high):
    return 2 * high + (label ^ (high // 2))


QUADS = [
    [place(a, zh) * SIDE + place(b, yh) for a in range(2) for b in range(2)]
    for zh in range(HALF)
    for yh in range(HALF)
]
QUAD_DEVICES = [
    [8 * r + k for r in sorted(quad)[::-1] for k in (5, 3, 7, 1, 0, 2, 4, 6)] for quad in QUADS
]
FAR = [
    [place(a, zh) * SIDE + place(b, yh) for zh in range(HALF) for yh in range(HALF)][::-1]
    for a in range(2)
    for b in range(2)
]


def one_row_of_quads():
    order = np.concatenate(
        [
            np.arange(32) + 32 * place(b, yh)
            for b in range(2)
            for yh in range(HALF)
        ]
    )
    return np.eye(256, dtype=np.float32)[:, order]


def nt(left, right):
    return lax.dot_general(
        left, right, (((1,), (1,)), ((), ())), preferred_element_type=jnp.float32
    )


def tn(left, right):
    return lax.dot_general(
        left, right, (((0,), (0,)), ((), ())), preferred_element_type=jnp.float32
    )


def nn(left, right):
    return jnp.dot(left, right, preferred_element_type=jnp.float32)


def my_label():
    me = lax.axis_index("rep")
    z, y = me // SIDE, lax.rem(me, SIDE)
    a = lax.rem(z, 2) ^ (z // HALF)
    b = lax.rem(y, 2) ^ (y // HALF)
    return 2 * a + b


def local_kernel(
    near, far, gain, pick, gate_w, up_hbm, down_hbm, own, sent_y, sent_z, sent_zy, keep, give,
    gain_sum, turned, up_w, down_w, gain_rows, sems,
):
    loads = [
        pltpu.make_async_copy(source, target, sems.at[k])
        for k, (source, target) in enumerate(((up_hbm, up_w), (down_hbm, down_w)))
    ]
    mine = my_label()

    once = jnp.minimum(mine, 0) + 1

    @pl.loop(0, once)
    def _(_):
        for load in loads:
            load.start()

    xf = jnp.concatenate((near[:, :2048], far[:, :2048]), axis=0).astype(jnp.float32)
    dy = jnp.concatenate((near[:, 2048:], far[:, 2048:]), axis=0)
    inv = lax.rsqrt(jnp.mean(xf * xf, axis=-1, keepdims=True) + EPS)
    normed = xf * inv
    hidden_in = (normed * gain[...]).astype(jnp.bfloat16)
    for z in range(SIDE):
        zh = z // 2
        a = (z % 2) ^ (zh // 2)
        block = nn(dy[:, 256 * z : 256 * z + 256], pick[...]).astype(jnp.bfloat16)
        for b in range(2):
            turned[2 * a + b, :, 128 * zh : 128 * zh + 128] = block[:, 128 * b : 128 * b + 128]
    gate = nt(hidden_in, gate_w[...])
    loads[0].wait()
    up = nt(hidden_in, up_w[...])
    sig = 1.0 / (1.0 + jnp.exp(-gate))
    act = gate * sig
    hidden = (act * up).astype(jnp.bfloat16)
    loads[1].wait()
    d_hidden = 0.5 * nt(dy, down_w[...])
    d_gate = (d_hidden * up * sig * (1.0 + gate * (1.0 - sig))).astype(jnp.bfloat16)
    d_up = (d_hidden * act).astype(jnp.bfloat16)
    part = nn(d_gate, gate_w[...]) + nn(d_up, up_w[...])
    keep[...] = part[:64]
    give[...] = part[64:].astype(jnp.bfloat16)
    total = jnp.sum(part * normed, axis=0, keepdims=True)
    rows = jnp.concatenate([total[:, 256 * k : 256 * k + 256] for k in range(8)], axis=0)
    for k in range(32):
        gain_rows[k] = rows.astype(jnp.bfloat16)
    store = pltpu.make_async_copy(gain_rows, gain_sum, sems.at[2])

    @pl.loop(0, once)
    def _(_):
        store.start()

    for k, out in enumerate((own, sent_y, sent_z, sent_zy)):
        out[:, :512] = turned[mine ^ k]
        out[:, 512:864] = hidden
        out[:, 864:] = jnp.zeros((128, 32), jnp.bfloat16)
    store.wait()


def reduce_kernel(own, got_y, got_z, got_zy, gains, blocks):
    part = tn(own[:, :512], own[:, 512:])
    for got in (got_y, got_z, got_zy):
        part = part + tn(got[:, :512], got[:, 512:])
    total = jnp.sum(gains[...].astype(jnp.float32), axis=0).astype(jnp.bfloat16)
    for k in range(16):
        mine = part[32 * k : 32 * k + 32]
        one, two, three, four = (mine[8 * j : 8 * j + 8, 256:352] for j in range(4))
        rest = jnp.concatenate(
            (
                jnp.concatenate((one, two[:, :32]), axis=1),
                jnp.concatenate((two[:, 32:], three[:, :64]), axis=1),
                jnp.concatenate((three[:, 64:], four), axis=1),
            ),
            axis=0,
        )
        blocks[15 - k, :32] = mine[:, :128].astype(jnp.bfloat16)
        blocks[15 - k, 32:64] = mine[:, 128:256].astype(jnp.bfloat16)
        blocks[15 - k, 64:88] = rest.astype(jnp.bfloat16)
        blocks[15 - k, 88:96] = total[:, :128]
        blocks[15 - k, 96:] = total[:, 128:]


def last_kernel(got, down, gain):
    total = got[0].astype(jnp.float32)
    for k in range(1, 16):
        total = total + got[k].astype(jnp.float32)
    one, two, three = (total[64 + 8 * j : 72 + 8 * j] for j in range(3))
    down[:, :128] = 0.5 * total[:32]
    down[:, 128:256] = 0.5 * total[32:64]
    down[:8, 256:] = 0.5 * one[:, :96]
    down[8:16, 256:] = 0.5 * jnp.concatenate((one[:, 96:], two[:, :64]), axis=1)
    down[16:24, 256:] = 0.5 * jnp.concatenate((two[:, 64:], three[:, :32]), axis=1)
    down[24:, 256:] = 0.5 * three[:, 32:]
    for k in range(8):
        for half in range(2):
            at = 256 * k + 128 * half
            gain[:, at : at + 128] = total[88 + 8 * half + k : 89 + 8 * half + k]


def split_kernel(keep, got, mine, to_one, to_two, to_three):
    me = lax.axis_index("fs")
    for k, out in enumerate((mine, to_one, to_two, to_three)):
        rows = pl.ds(pl.multiple_of(16 * (me ^ k ^ FIRST_CHIP), 16), 16)
        out[...] = (keep[rows, :] + got[rows, :].astype(jnp.float32)).astype(out.dtype)


def input_kernel(mine, from_one, from_two, from_three, inputs, gain, out):
    d_in = mine[...]
    for got in (from_one, from_two, from_three):
        d_in = d_in + got[...].astype(jnp.float32)
    xf = inputs[...].astype(jnp.float32)
    inv = lax.rsqrt(jnp.mean(xf * xf, axis=-1, keepdims=True) + EPS)
    normed = xf * inv
    scaled = d_in * gain[...]
    mean = jnp.mean(scaled * normed, axis=-1, keepdims=True)
    out[...] = (inv * (scaled - normed * mean)).astype(out.dtype)


def call(body, shapes, *args, scratch=(), flops=1000000, vmem=16, left=0, last=0):
    whole = pl.BlockSpec(memory_space=pltpu.VMEM)
    far = pl.BlockSpec(memory_space=pltpu.HBM)
    out = [jax.ShapeDtypeStruct(s, t) for s, t in shapes]
    return pl.pallas_call(
        body,
        out_shape=out,
        in_specs=[whole] * (len(args) - left) + [far] * left,
        out_specs=[whole] * (len(out) - last) + [far] * last,
        scratch_shapes=scratch,
        cost_estimate=pl.CostEstimate(flops=flops, bytes_accessed=4000000, transcendentals=0),
        compiler_params=pltpu.CompilerParams(vmem_limit_bytes=vmem * 2**20),
    )(*args)


def partner(array, axis, bit):
    count = lax.axis_size(axis)
    return lax.ppermute(array, axis, [(i, i ^ bit) for i in range(count)])


def per_device(inputs, cotangent, norm_gain, gate_weight, up_weight, down_weight):
    own = jnp.concatenate((inputs, cotangent), axis=1)
    near = lax.all_to_all(
        jnp.broadcast_to(own[None], (4, *own.shape)),
        "fs",
        0,
        0,
        tiled=True,
        axis_index_groups=[[k ^ FIRST_CHIP for k in range(4)]],
    ).reshape(64, 4096)
    other = partner(near, "tp", 1)
    pick = jnp.asarray(one_row_of_quads(), jnp.bfloat16)
    block = ((128, 896), jnp.bfloat16)
    own, sent_y, sent_z, sent_zy, keep, give, part_gain = call(
        local_kernel,
        [
            block,
            block,
            block,
            block,
            ((64, 2048), jnp.float32),
            ((64, 2048), jnp.bfloat16),
            ((32, 8, 256), jnp.bfloat16),
        ],
        near,
        other,
        norm_gain.reshape(1, 2048),
        pick,
        gate_weight.T,
        pltpu.with_memory_space_constraint(up_weight.T, pltpu.HBM),
        pltpu.with_memory_space_constraint(down_weight, pltpu.HBM),
        scratch=[
            pltpu.VMEM((4, 128, 512), jnp.bfloat16),
            pltpu.VMEM((352, 2048), jnp.bfloat16),
            pltpu.VMEM((352, 2048), jnp.bfloat16),
            pltpu.VMEM((32, 8, 256), jnp.bfloat16),
            pltpu.SemaphoreType.DMA((3,)),
        ],
        flops=1000000000,
        vmem=32,
        left=2,
        last=1,
    )

    gains = lax.all_to_all(
        part_gain, EVERY, 0, 0, tiled=True, axis_index_groups=QUAD_DEVICES
    )
    got_zy = partner(sent_zy, "rep", SIDE + 1)
    got_z = partner(sent_z, "rep", SIDE)
    got_y = partner(sent_y, "rep", 1)
    (blocks,) = call(
        reduce_kernel,
        [((16, 104, 128), jnp.bfloat16)],
        own,
        got_y,
        got_z,
        got_zy,
        gains,
    )
    got = lax.all_to_all(blocks, "rep", 0, 0, tiled=True, axis_index_groups=FAR)
    down, gain = call(last_kernel, [((32, 352), jnp.float32), ((1, 2048), jnp.float32)], got)
    down_grad = down.T
    gain_grad = gain.reshape(2048)

    got = partner(give, "tp", 1)
    tokens = ((16, 2048), jnp.bfloat16)
    mine, *sends = call(
        split_kernel, [((16, 2048), jnp.float32), tokens, tokens, tokens], keep, got
    )
    gots = []
    for k in range(3):
        gots.append(partner(sends[k], "fs", k + 1))
    (input_grad,) = call(
        input_kernel, [tokens], mine, *gots, inputs, norm_gain.reshape(1, 2048)
    )
    return (input_grad, gain_grad, down_grad)


def solution(mesh):
    placed = (
        P(EVERY, None),
        P(EVERY, None),
        P(),
        P(None, OWN),
        P(None, OWN),
        P(OWN, None),
    )

    return jax.shard_map(
        per_device,
        mesh=mesh,
        in_specs=placed,
        out_specs=(P(EVERY, None), P(), P(OWN, "rep")),
        check_vma=False,
    )
```

```python
import jax
import jax.numpy as jnp
import numpy as np
from jax import lax
from jax.experimental import pallas as pl
from jax.experimental.pallas import tpu as pltpu
from jax.sharding import PartitionSpec as P


EPS = 1e-06
SIDE = 8
HALF = SIDE // 2
FIRST_CHIP = 3
EVERY = ("rep", "fs", "tp")
OWN = ("fs", "tp")


def place(label, high):
    return 2 * high + (label ^ (high // 2))


QUADS = [
    [place(a, zh) * SIDE + place(b, yh) for a in range(2) for b in range(2)]
    for zh in range(HALF)
    for yh in range(HALF)
]
QUAD_DEVICES = [
    [8 * r + k for r in sorted(quad)[::-1] for k in (5, 3, 7, 1, 0, 2, 4, 6)] for quad in QUADS
]
FAR_ORDER = tuple(HALF * zh + yh for yh in (3, 2, 1, 0) for zh in (3, 2, 1, 0))
FAR = [
    [place(a, k // HALF) * SIDE + place(b, k % HALF) for k in FAR_ORDER]
    for a in range(2)
    for b in range(2)
]
PLACES = [FAR_ORDER.index(k) for k in range(HALF * HALF)]


def one_row_of_quads():
    order = np.concatenate(
        [
            np.arange(32) + 32 * place(b, yh)
            for b in range(2)
            for yh in range(HALF)
        ]
    )
    return np.eye(256, dtype=np.float32)[:, order]


def nt(left, right):
    return lax.dot_general(
        left, right, (((1,), (1,)), ((), ())), preferred_element_type=jnp.float32
    )


def tn(left, right):
    return lax.dot_general(
        left, right, (((0,), (0,)), ((), ())), preferred_element_type=jnp.float32
    )


def nn(left, right):
    return jnp.dot(left, right, preferred_element_type=jnp.float32)


def my_label():
    me = lax.axis_index("rep")
    z, y = me // SIDE, lax.rem(me, SIDE)
    a = lax.rem(z, 2) ^ (z // HALF)
    b = lax.rem(y, 2) ^ (y // HALF)
    return 2 * a + b


def local_kernel(
    near, far, gain, pick, gate_w, up_hbm, down_hbm, own, sent_y, sent_z, sent_zy, keep, give,
    gain_sum, turned, up_w, down_w, gain_rows, sems,
):
    loads = [
        pltpu.make_async_copy(source, target, sems.at[k])
        for k, (source, target) in enumerate(((up_hbm, up_w), (down_hbm, down_w)))
    ]
    mine = my_label()

    once = jnp.minimum(mine, 0) + 1

    @pl.loop(0, once)
    def _(_):
        for load in loads:
            load.start()

    xf = jnp.concatenate((near[:, :2048], far[:, :2048]), axis=0).astype(jnp.float32)
    dy = jnp.concatenate((near[:, 2048:], far[:, 2048:]), axis=0)
    inv = lax.rsqrt(jnp.mean(xf * xf, axis=-1, keepdims=True) + EPS)
    normed = xf * inv
    hidden_in = (normed * gain[...]).astype(jnp.bfloat16)
    for z in range(SIDE):
        zh = z // 2
        a = (z % 2) ^ (zh // 2)
        block = nn(dy[:, 256 * z : 256 * z + 256], pick[...]).astype(jnp.bfloat16)
        for b in range(2):
            turned[2 * a + b, :, 128 * zh : 128 * zh + 128] = block[:, 128 * b : 128 * b + 128]
    gate = nt(hidden_in, gate_w[...])
    loads[0].wait()
    up = nt(hidden_in, up_w[...])
    sig = 1.0 / (1.0 + jnp.exp(-gate))
    act = gate * sig
    hidden = (act * up).astype(jnp.bfloat16)
    loads[1].wait()
    d_hidden = 0.5 * nt(dy, down_w[...])
    d_gate = (d_hidden * up * sig * (1.0 + gate * (1.0 - sig))).astype(jnp.bfloat16)
    d_up = (d_hidden * act).astype(jnp.bfloat16)
    part = nn(d_gate, gate_w[...]) + nn(d_up, up_w[...])
    keep[...] = part[:64]
    give[...] = part[64:].astype(jnp.bfloat16)
    total = jnp.sum(part * normed, axis=0, keepdims=True)
    rows = jnp.concatenate([total[:, 256 * k : 256 * k + 256] for k in range(8)], axis=0)
    for k in range(32):
        gain_rows[k] = rows.astype(jnp.bfloat16)
    store = pltpu.make_async_copy(gain_rows, gain_sum, sems.at[2])

    @pl.loop(0, once)
    def _(_):
        store.start()

    for k, out in enumerate((own, sent_y, sent_z, sent_zy)):
        out[:, :512] = turned[mine ^ k]
        out[:, 512:864] = hidden
        out[:, 864:] = jnp.zeros((128, 32), jnp.bfloat16)
    store.wait()


def reduce_kernel(own, got_y, got_z, got_zy, gains, blocks):
    part = tn(own[:, :512], own[:, 512:])
    for got in (got_y, got_z, got_zy):
        part = part + tn(got[:, :512], got[:, 512:])
    total = jnp.sum(gains[...].astype(jnp.float32), axis=0).astype(jnp.bfloat16)
    for k in range(16):
        mine = part[32 * k : 32 * k + 32]
        one, two, three, four = (mine[8 * j : 8 * j + 8, 256:352] for j in range(4))
        rest = jnp.concatenate(
            (
                jnp.concatenate((one, two[:, :32]), axis=1),
                jnp.concatenate((two[:, 32:], three[:, :64]), axis=1),
                jnp.concatenate((three[:, 64:], four), axis=1),
            ),
            axis=0,
        )
        blocks[PLACES[k], :32] = mine[:, :128].astype(jnp.bfloat16)
        blocks[PLACES[k], 32:64] = mine[:, 128:256].astype(jnp.bfloat16)
        blocks[PLACES[k], 64:88] = rest.astype(jnp.bfloat16)
        blocks[PLACES[k], 88:96] = total[:, :128]
        blocks[PLACES[k], 96:] = total[:, 128:]


def last_kernel(got, down, gain):
    total = got[0].astype(jnp.float32)
    for k in range(1, 16):
        total = total + got[k].astype(jnp.float32)
    one, two, three = (total[64 + 8 * j : 72 + 8 * j] for j in range(3))
    down[:, :128] = 0.5 * total[:32]
    down[:, 128:256] = 0.5 * total[32:64]
    down[:8, 256:] = 0.5 * one[:, :96]
    down[8:16, 256:] = 0.5 * jnp.concatenate((one[:, 96:], two[:, :64]), axis=1)
    down[16:24, 256:] = 0.5 * jnp.concatenate((two[:, 64:], three[:, :32]), axis=1)
    down[24:, 256:] = 0.5 * three[:, 32:]
    for k in range(8):
        for half in range(2):
            at = 256 * k + 128 * half
            gain[:, at : at + 128] = total[88 + 8 * half + k : 89 + 8 * half + k]


def split_kernel(keep, got, mine, to_one, to_two, to_three):
    me = lax.axis_index("fs")
    for k, out in enumerate((mine, to_one, to_two, to_three)):
        rows = pl.ds(pl.multiple_of(16 * (me ^ k ^ FIRST_CHIP), 16), 16)
        out[...] = (keep[rows, :] + got[rows, :].astype(jnp.float32)).astype(out.dtype)


def input_kernel(mine, from_one, from_two, from_three, inputs, gain, out):
    d_in = mine[...]
    for got in (from_one, from_two, from_three):
        d_in = d_in + got[...].astype(jnp.float32)
    xf = inputs[...].astype(jnp.float32)
    inv = lax.rsqrt(jnp.mean(xf * xf, axis=-1, keepdims=True) + EPS)
    normed = xf * inv
    scaled = d_in * gain[...]
    mean = jnp.mean(scaled * normed, axis=-1, keepdims=True)
    out[...] = (inv * (scaled - normed * mean)).astype(out.dtype)


def call(body, shapes, *args, scratch=(), flops=1000000, vmem=16, left=0, last=0):
    whole = pl.BlockSpec(memory_space=pltpu.VMEM)
    far = pl.BlockSpec(memory_space=pltpu.HBM)
    out = [jax.ShapeDtypeStruct(s, t) for s, t in shapes]
    return pl.pallas_call(
        body,
        out_shape=out,
        in_specs=[whole] * (len(args) - left) + [far] * left,
        out_specs=[whole] * (len(out) - last) + [far] * last,
        scratch_shapes=scratch,
        cost_estimate=pl.CostEstimate(flops=flops, bytes_accessed=4000000, transcendentals=0),
        compiler_params=pltpu.CompilerParams(vmem_limit_bytes=vmem * 2**20),
    )(*args)


def partner(array, axis, bit):
    count = lax.axis_size(axis)
    return lax.ppermute(array, axis, [(i, i ^ bit) for i in range(count)])


def per_device(inputs, cotangent, norm_gain, gate_weight, up_weight, down_weight):
    own = jnp.concatenate((inputs, cotangent), axis=1)
    near = lax.all_to_all(
        jnp.broadcast_to(own[None], (4, *own.shape)),
        "fs",
        0,
        0,
        tiled=True,
        axis_index_groups=[[k ^ FIRST_CHIP for k in range(4)]],
    ).reshape(64, 4096)
    other = partner(near, "tp", 1)
    pick = jnp.asarray(one_row_of_quads(), jnp.bfloat16)
    block = ((128, 896), jnp.bfloat16)
    own, sent_y, sent_z, sent_zy, keep, give, part_gain = call(
        local_kernel,
        [
            block,
            block,
            block,
            block,
            ((64, 2048), jnp.float32),
            ((64, 2048), jnp.bfloat16),
            ((32, 8, 256), jnp.bfloat16),
        ],
        near,
        other,
        norm_gain.reshape(1, 2048),
        pick,
        gate_weight.T,
        pltpu.with_memory_space_constraint(up_weight.T, pltpu.HBM),
        pltpu.with_memory_space_constraint(down_weight, pltpu.HBM),
        scratch=[
            pltpu.VMEM((4, 128, 512), jnp.bfloat16),
            pltpu.VMEM((352, 2048), jnp.bfloat16),
            pltpu.VMEM((352, 2048), jnp.bfloat16),
            pltpu.VMEM((32, 8, 256), jnp.bfloat16),
            pltpu.SemaphoreType.DMA((3,)),
        ],
        flops=1000000000,
        vmem=32,
        left=2,
        last=1,
    )

    gains = lax.all_to_all(
        part_gain, EVERY, 0, 0, tiled=True, axis_index_groups=QUAD_DEVICES
    )
    got_zy = partner(sent_zy, "rep", SIDE + 1)
    got_z = partner(sent_z, "rep", SIDE)
    got_y = partner(sent_y, "rep", 1)
    (blocks,) = call(
        reduce_kernel,
        [((16, 104, 128), jnp.bfloat16)],
        own,
        got_y,
        got_z,
        got_zy,
        gains,
    )
    got = lax.all_to_all(blocks, "rep", 0, 0, tiled=True, axis_index_groups=FAR)
    down, gain = call(last_kernel, [((32, 352), jnp.float32), ((1, 2048), jnp.float32)], got)
    down_grad = down.T
    gain_grad = gain.reshape(2048)

    got = partner(give, "tp", 1)
    tokens = ((16, 2048), jnp.bfloat16)
    mine, *sends = call(
        split_kernel, [((16, 2048), jnp.float32), tokens, tokens, tokens], keep, got
    )
    gots = []
    for k in range(3):
        gots.append(partner(sends[k], "fs", k + 1))
    (input_grad,) = call(
        input_kernel, [tokens], mine, *gots, inputs, norm_gain.reshape(1, 2048)
    )
    return (input_grad, gain_grad, down_grad)


def solution(mesh):
    placed = (
        P(EVERY, None),
        P(EVERY, None),
        P(),
        P(None, OWN),
        P(None, OWN),
        P(OWN, None),
    )

    return jax.shard_map(
        per_device,
        mesh=mesh,
        in_specs=placed,
        out_specs=(P(EVERY, None), P(), P(OWN, "rep")),
        check_vma=False,
    )
```
